32 devices in a mesh: sp: 8 (over z, x), tp: 4 (over y, core).
Axes of the slice: x: 2, y: 2, z: 4, core: 2. Of those that a mesh axis runs over, the one named last changes fastest.
Arguments:
- tokens: bfloat16 [3072, 2048], P('sp', 'tp'), may hold values from -6 to 6
- ret_query: bfloat16 [2048, 1024], P(None, 'tp'), may hold values from -0.125 to 0.125
- ret_key: bfloat16 [2048, 1024], P(None, 'tp'), may hold values from -0.125 to 0.125
- ret_value: bfloat16 [2048, 1024], P(None, 'tp'), may hold values from -0.125 to 0.125
- stick_query: bfloat16 [2048, 1024], P(None, 'tp'), may hold values from -0.125 to 0.125
- stick_key: bfloat16 [2048, 1024], P(None, 'tp'), may hold values from -0.125 to 0.125
- stick_value: bfloat16 [2048, 1024], P(None, 'tp'), may hold values from -0.125 to 0.125
- log_decay: float32 [3072, 8], P('sp', 'tp'), may hold values from -1.2 to 0
- stick_bias: float32 [8], P('tp'), may hold values from -13 to -5
- out_ret: bfloat16 [1024, 2048], P('tp'), may hold values from -0.125 to 0.125
- out_stick: bfloat16 [1024, 2048], P('tp'), may hold values from -0.125 to 0.125
Outputs:
- mixed: bfloat16 [3072, 2048], P('sp', 'tp')
The draws below stay inside these ranges and needn't reach their ends.
All inputs are finite; a program needn't handle non-finite values.
Results may differ from the reference program's by a relative error of at most 0.019.
Values may be sent and summed in bfloat16 or wider, within the bound.
A program may use at most 64 MiB of HBM per device.

```python
import jax
import jax.numpy as jnp
from jax import lax

D = 2048
HEAD_DIM = 128
RET_HEADS = 8
SB_HEADS = 8
TOK_DEV = 384
TOKENS = 3072


def draw_log_decay(key, part):
    streams = jax.random.split(key, 7)
    slow_share = 0.5
    base_rate = jax.random.uniform(streams[0], (RET_HEADS,), jnp.float32, 0.2, 0.5)
    slow_heads = jax.random.bernoulli(streams[1], slow_share, (RET_HEADS,))
    fast_rate = jax.random.uniform(streams[2], (RET_HEADS,), jnp.float32, 1.0 / 60.0, 1.0 / 30.0)
    head_decay_rate = jnp.where(slow_heads, base_rate / TOKENS, fast_rate)
    block_count = TOKENS // TOK_DEV
    block_multiplier = jnp.exp(jax.random.uniform(streams[3], (block_count, RET_HEADS), jnp.float32, -0.69, 0.69))
    block_multiplier = jnp.repeat(block_multiplier, TOK_DEV, axis=0)
    jaggedness = jnp.exp(jax.random.uniform(streams[4], (TOKENS, RET_HEADS), jnp.float32, -0.5, 0.47))
    location_list = jax.random.randint(streams[5], (2, RET_HEADS), 0, TOKENS)
    loss_values = jax.random.uniform(streams[6], (2, RET_HEADS), jnp.float32, 0.2, 0.4)
    row_position_index = jnp.arange(TOKENS, dtype=jnp.int32)[:, None]
    spike_groups = jnp.where(row_position_index == location_list[0][None, :], jnp.log(1.0 - loss_values[0])[None, :], 0.0)
    spike_groups = spike_groups + jnp.where(row_position_index == location_list[1][None, :], jnp.log(1.0 - loss_values[1])[None, :], 0.0)
    return (-head_decay_rate[None, :] * block_multiplier * jaggedness + spike_groups).astype(jnp.float32)


def draw_stick_bias(key, part):
    return jax.random.uniform(key, (SB_HEADS,), jnp.float32, -13.0, -5.0)


def block_levels(own_key, shape, pieces, smallest, high):
    def one(position, parts):
        draws = jax.random.uniform(jax.random.fold_in(jax.random.fold_in(own_key, 6), position), (parts,), jnp.float32, smallest / len(pieces), high / len(pieces))
        return jnp.repeat(jnp.exp(draws), shape[position] // parts).reshape((-1,) + (1,) * (len(shape) - position - 1))

    loudness = one(*pieces[0])
    for cut in pieces[1:]:
        loudness = loudness * one(*cut)
    return loudness


def scatter_about(key, extent, scale, bound, shards=(), kind=jnp.bfloat16):
    loudness = block_levels(key, extent, shards, -0.22, 0.18) if shards else 1.0
    entries = jax.random.normal(key, extent, jnp.float32) * scale * loudness
    return jnp.minimum(jnp.maximum(entries, -bound), bound).astype(kind)


def setup_inputs(seed: int = 0) -> dict:
    seeds = jax.random.split(jax.random.key(seed), 12)
    tokens = scatter_about(seeds[0], (TOKENS, D), 1.0, 6.0, ((0, 8), (1, 4)))
    ret_query = scatter_about(seeds[1], (D, RET_HEADS * HEAD_DIM), D ** -0.5, 0.125, ((1, 4),))
    ret_key = scatter_about(seeds[2], (D, RET_HEADS * HEAD_DIM), D ** -0.5, 0.125, ((1, 4),))
    ret_value = scatter_about(seeds[3], (D, RET_HEADS * HEAD_DIM), D ** -0.5, 0.125, ((1, 4),))
    stick_query = scatter_about(seeds[4], (D, SB_HEADS * HEAD_DIM), D ** -0.5, 0.125, ((1, 4),))
    stick_key = scatter_about(seeds[5], (D, SB_HEADS * HEAD_DIM), D ** -0.5, 0.125, ((1, 4),))
    stick_value = scatter_about(seeds[6], (D, SB_HEADS * HEAD_DIM), D ** -0.5, 0.125, ((1, 4),))
    log_decay = draw_log_decay(jax.random.fold_in(seeds[11], 71), 0)
    stick_bias = draw_stick_bias(jax.random.fold_in(seeds[11], 71), 0)
    out_ret = scatter_about(seeds[9], (RET_HEADS * HEAD_DIM, D), ((RET_HEADS + SB_HEADS) * HEAD_DIM) ** -0.5, 0.125, ((0, 4),))
    out_stick = scatter_about(seeds[10], (SB_HEADS * HEAD_DIM, D), ((RET_HEADS + SB_HEADS) * HEAD_DIM) ** -0.5, 0.125, ((0, 4),))
    return dict(tokens=tokens, ret_query=ret_query, ret_key=ret_key, ret_value=ret_value, stick_query=stick_query, stick_key=stick_key, stick_value=stick_value, log_decay=log_decay, stick_bias=stick_bias, out_ret=out_ret, out_stick=out_stick)


EPS = 1e-05
ROPE_BASE = 10000.0

def rounded(values):
    return lax.optimization_barrier(values.astype(jnp.bfloat16)).astype(jnp.float32)

def rotate(values, positions):
    half_width = values.shape[-1] // 2
    inverse = ROPE_BASE ** (-jnp.arange(half_width, dtype=jnp.float32) / half_width)
    angles = positions[:, None] * inverse[None, :]
    cosine = jnp.cos(angles)[:, None, :]
    sine_part = jnp.sin(angles)[:, None, :]
    first_half = values[..., :half_width]
    second_half = values[..., half_width:]
    return jnp.concatenate([first_half * cosine - second_half * sine_part, first_half * sine_part + second_half * cosine], axis=-1)

def head_norm(values):
    centred = values - lax.optimization_barrier(jnp.mean(values, axis=-1, keepdims=True))
    spread = lax.optimization_barrier(jnp.mean(centred * centred, axis=-1, keepdims=True))
    return centred * lax.rsqrt(spread + EPS)

def retention(query_rot, key_rot, value_rows, log_decay):
    blocks = TOKENS // TOK_DEV
    head_count = query_rot.shape[1]
    index_rows = jnp.arange(TOK_DEV, dtype=jnp.int32)
    lower = (index_rows[:, None] >= index_rows[None, :])[None]

    def split(values):
        return values.reshape((blocks, TOK_DEV) + values.shape[1:])

    def advance(state, block):
        query_block, key_block, value_block, decay_block = block
        cumulative = jnp.cumsum(decay_block, axis=0)
        final_decay = cumulative[-1]
        gaps = cumulative.T[:, :, None] - cumulative.T[:, None, :]
        decay = jnp.where(lower, jnp.exp(jnp.where(lower, gaps, 0.0)), 0.0)
        scores = jnp.einsum('thd,shd->hts', query_block.astype(jnp.float32), key_block.astype(jnp.float32))
        inner = rounded(scores * decay)
        local_part = jnp.einsum('hts,she->the', inner, value_block.astype(jnp.float32))
        carried = jnp.einsum('thd,hde->the', query_block.astype(jnp.float32), state, precision=lax.Precision.HIGHEST) * jnp.exp(cumulative)[:, :, None]
        weighted = rounded(key_block.astype(jnp.float32) * jnp.exp(final_decay[None, :] - cumulative)[:, :, None])
        fresh = jnp.einsum('shd,she->hde', weighted, value_block.astype(jnp.float32))
        state = jnp.exp(final_decay)[:, None, None] * state + fresh
        return (state, local_part + carried)
    start_state = jnp.zeros((head_count, HEAD_DIM, HEAD_DIM), jnp.float32)
    _, outputs = lax.scan(advance, start_state, (split(query_rot), split(key_rot), split(value_rows), split(log_decay)))
    return outputs.reshape(TOKENS, head_count, HEAD_DIM)

def stick_breaking(queries, keys, values, bias):
    blocks = TOKENS // TOK_DEV
    head_count = queries.shape[1]
    scale = HEAD_DIM ** (-0.5)
    keys_heads = jnp.transpose(keys, (1, 0, 2)).astype(jnp.float32)
    values_heads = jnp.transpose(values, (1, 0, 2)).astype(jnp.float32).reshape(head_count, blocks, TOK_DEV, HEAD_DIM)
    key_pos = jnp.arange(TOKENS, dtype=jnp.int32)

    def one_block(index):
        block_queries = lax.dynamic_slice_in_dim(queries, index * TOK_DEV, TOK_DEV, 0)
        query_heads = jnp.transpose(block_queries, (1, 0, 2)).astype(jnp.float32)
        query_pos = index * TOK_DEV + jnp.arange(TOK_DEV, dtype=jnp.int32)
        visible = (key_pos[None, :] < query_pos[:, None]).reshape(TOK_DEV, blocks, TOK_DEV)

        def one_head(query_h, key_h, value_h, bias_h):
            logits = (jnp.dot(query_h, key_h.T) * scale + bias_h).reshape(TOK_DEV, blocks, TOK_DEV)
            success = jax.nn.log_sigmoid(logits)
            failure = jnp.where(visible, success - logits, 0.0)
            suffix = lax.cumsum(failure, axis=2, reverse=True) - failure
            weights = rounded(jnp.where(visible, jnp.exp(success + suffix), 0.0))
            partial_value = jnp.einsum('tpk,pke->tpe', weights, value_h)
            totals = lax.optimization_barrier(jnp.sum(failure, axis=2))
            behind = lax.cumsum(totals, axis=1, reverse=True) - totals
            return lax.optimization_barrier(jnp.sum(jnp.exp(behind)[:, :, None] * partial_value, axis=1))
        return jax.vmap(one_head)(query_heads, keys_heads, values_heads, bias)
    outputs = lax.map(one_block, jnp.arange(blocks, dtype=jnp.int32))
    return jnp.transpose(outputs, (0, 2, 1, 3)).reshape(TOKENS, head_count, HEAD_DIM)

def reference(tokens, ret_query, ret_key, ret_value, stick_query, stick_key, stick_value, log_decay, stick_bias, out_ret, out_stick):

    def project(matrix):
        return jnp.dot(tokens, matrix, preferred_element_type=jnp.float32).astype(jnp.bfloat16).reshape(TOKENS, -1, HEAD_DIM)
    positions = jnp.arange(TOKENS, dtype=jnp.float32)
    query_rot = rotate(project(ret_query).astype(jnp.float32), positions).astype(jnp.bfloat16)
    key_rot = (rotate(project(ret_key).astype(jnp.float32), positions) * HEAD_DIM ** (-0.5)).astype(jnp.bfloat16)
    ret_out = head_norm(retention(query_rot, key_rot, project(ret_value), log_decay)).astype(jnp.bfloat16)
    stick_out = head_norm(stick_breaking(project(stick_query), project(stick_key), project(stick_value), stick_bias)).astype(jnp.bfloat16)
    mixed = jnp.dot(ret_out.reshape(TOKENS, -1), out_ret, preferred_element_type=jnp.float32)
    mixed = mixed + jnp.dot(stick_out.reshape(TOKENS, -1), out_stick, preferred_element_type=jnp.float32)
    return mixed.astype(jnp.bfloat16)
```

```python
import functools

import jax
import jax.numpy as jnp
from jax import lax
from jax.experimental import pallas as pl
from jax.experimental.pallas import tpu as pltpu
from jax.sharding import PartitionSpec as P

HEAD_DIM = 128
EPS = 1e-05
ROPE_BASE = 10000.0
CORES = 2
F32 = jnp.float32
BF16 = jnp.bfloat16


def row_width(shards):
    width = 1
    while (2 * width) ** 2 <= shards and shards % (2 * width) == 0:
        width *= 2
    return width


def head_norm(values):
    centred = values - jnp.mean(values, axis=-1, keepdims=True)
    spread = jnp.mean(centred * centred, axis=-1, keepdims=True)
    return centred * lax.rsqrt(spread + EPS)


def nt(a, b):
    return lax.dot_general(a, b, (((1,), (1,)), ((), ())), preferred_element_type=F32)


def dot(a, b):
    return jnp.dot(a, b, preferred_element_type=F32)


def kernel(
    shards,
    parts,
    tok,
    w_rq,
    w_rk,
    w_rv,
    w_sq,
    w_sk,
    w_sv,
    o_ret,
    o_stick,
    log_decay,
    cos_t,
    sin_t,
    bias,
    out,
    xs,
    wall,
    wo,
    acc,
    kv,
    sq,
    qrot,
    retv,
    local,
    tri,
    cumb,
    fresh,
    st_in,
    st_out,
    running,
    trailing,
    feats,
    d_send,
    d_recv,
    y_send,
    y_recv,
    w_sem,
    tok_sem,
    own_s,
    own_r,
    fwd_s,
    fwd_r,
    kv_s,
    kv_r,
    st_s,
    st_r,
    dd_s,
    dd_r,
    yy_s,
    yy_r,
):
    rows, depth = tok.shape
    width = w_rq.shape[1]
    heads = width // HEAD_DIM
    chips = parts // CORES
    across = row_width(shards)
    me = lax.axis_index("sp")
    t = lax.axis_index("tp")
    chip = t // CORES
    core = t % CORES
    partner = chip * CORES + (1 - core)
    column = me % across
    first = me - column
    chunk = 128 if rows % 128 == 0 else rows
    chunks = rows // chunk
    scale = HEAD_DIM ** (-0.5)

    def tp_at(off):
        return lax.rem(chip + off + chips, chips) * CORES + core

    def at(sp_index, tp_index):
        return {"sp": sp_index, "tp": tp_index}

    order = (w_sk, w_sv, w_sq, w_rk, w_rv, w_rq)
    own_load = pltpu.make_async_copy(tok, xs.at[t], tok_sem)
    own_load.start()
    loads = []
    for i, w in enumerate(order):
        load = pltpu.make_async_copy(w, wall.at[:, pl.ds(i * width, width)], w_sem.at[i])
        load.start()
        loads.append(load)
    out_loads = []
    for i, w in enumerate((o_ret, o_stick)):
        load = pltpu.make_async_copy(w, wo.at[pl.ds(i * width, width), :], w_sem.at[6 + i])
        load.start()
        out_loads.append(load)

    barrier = pltpu.get_barrier_semaphore()

    def greet(sp_index, tp_index):
        pl.semaphore_signal(
            barrier, inc=1, device_id=at(sp_index, tp_index), device_id_type=pl.DeviceIdType.MESH
        )

    greet(me, partner)
    for off in range(1, chips):
        greet(me, tp_at(off))
    for off in range(1, across):
        greet(first + lax.rem(column + off, across), t)
    count = 1 + (chips - 1) + (across - 1)
    for step in (across, 1):
        up = me + step < shards
        down = me - step >= 0

        @pl.when(up)
        def _():
            greet(me + step, t)

        @pl.when(down)
        def _():
            greet(me - step, t)

        count = count + up.astype(jnp.int32) + down.astype(jnp.int32)
    pl.semaphore_wait(barrier, count)

    def remote(src, dst, send, recv, sp_index, tp_index):
        return pltpu.make_async_remote_copy(
            src_ref=src,
            dst_ref=dst,
            send_sem=send,
            recv_sem=recv,
            device_id=at(sp_index, tp_index),
            device_id_type=pl.DeviceIdType.MESH,
        )

    sends = []
    for off in range(1, chips):
        copy = remote(tok, xs.at[t], own_s.at[off], own_r.at[off], me, tp_at(off))
        copy.start()
        sends.append(copy)
    near = remote(tok, xs.at[t], own_s.at[0], own_r.at[0], me, partner)
    near.start()

    lane = lax.broadcasted_iota(jnp.int32, (rows, rows), 1)
    sub = lax.broadcasted_iota(jnp.int32, (rows, rows), 0)
    tri[...] = (sub > lane).astype(BF16)
    for h in range(heads):
        column_ld = jnp.broadcast_to(log_decay[:, h : h + 1], (rows, rows))
        cum_row = jnp.sum(jnp.where(sub <= lane, column_ld, 0.0), axis=0, keepdims=True)
        ld_row = jnp.sum(jnp.where(sub == lane, column_ld, 0.0), axis=0, keepdims=True)
        cum_col = jnp.sum(
            jnp.where(lane <= sub, jnp.broadcast_to(ld_row, (rows, rows)), 0.0),
            axis=1,
            keepdims=True,
        )
        gaps = cum_col - cum_row
        acc[:, pl.ds(h * rows, rows)] = jnp.where(
            lane <= sub, jnp.exp(jnp.where(lane <= sub, gaps, 0.0)), 0.0
        )
        cumb[h] = jnp.broadcast_to(cum_col, (rows, HEAD_DIM))
    for h in range(heads):
        local[h] = acc[:, pl.ds(h * rows, rows)]

    own_load.wait()
    for load in loads:
        load.wait()

    def weight(j, lo, size):
        return wall[pl.ds(pl.multiple_of(j * depth, depth), depth), pl.ds(lo, size)]

    total = 6 * width
    for i in range(3):
        lo = i * 2 * width
        acc[:, pl.ds(lo, 2 * width)] = dot(xs[t], weight(t, lo, 2 * width))
    near.wait_recv()
    for i in range(3):
        lo = i * 2 * width
        acc[:, pl.ds(lo, 2 * width)] += dot(xs[partner], weight(partner, lo, 2 * width))
    forwards = []
    for off in range(1, chips):
        sends[off - 1].wait_recv()
        j = tp_at(-off)
        copy = remote(xs.at[j], xs.at[j], fwd_s.at[off], fwd_r.at[off], me, partner)
        copy.start()
        forwards.append(copy)
        for i in range(3):
            lo = i * 2 * width
            acc[:, pl.ds(lo, 2 * width)] += dot(xs[j], weight(j, lo, 2 * width))
    far = []
    for off in range(1, chips):
        forwards[off - 1].wait_recv()
        j = tp_at(-off) // CORES * CORES + (1 - core)
        far.append(j)

    def finish(lo, size):
        value = acc[:, pl.ds(lo, size)]
        for j in far:
            value = value + dot(xs[j], weight(j, lo, size))
        return value

    kv[me, 0] = finish(0, width).astype(BF16)
    kv[me, 1] = finish(width, width).astype(BF16)

    def block_copy(b, slot, target):
        return remote(kv.at[b], kv.at[b], kv_s.at[b, slot], kv_r.at[b], target, t)

    def spread(b, act):
        mine = lax.rem(b, across) == column

        @pl.when(jnp.logical_and(mine, me + across < shards))
        def _():
            act(block_copy(b, 0, me + across))

        for off in range(1, across):
            target = first + lax.rem(column + off, across)

            @pl.when(jnp.logical_and(mine, jnp.logical_or(b < me, target > me)))
            def _():
                act(block_copy(b, off, target))

    spread(me, lambda copy: copy.start())

    sq[...] = finish(2 * width, width).astype(BF16)
    rk = finish(3 * width, width).astype(BF16).astype(F32)
    retv[...] = finish(4 * width, width).astype(BF16)
    rq = finish(5 * width, width).astype(BF16).astype(F32)
    cos, sin = cos_t[...], sin_t[...]
    for h in range(heads):
        part = slice(h * HEAD_DIM, (h + 1) * HEAD_DIM)
        q, k = rq[:, part], rk[:, part]
        q = (q * cos + pltpu.roll(q, HEAD_DIM // 2, 1) * sin).astype(BF16)
        k = ((k * cos + pltpu.roll(k, HEAD_DIM // 2, 1) * sin) * scale).astype(BF16)
        qrot[h] = q
        v = retv[:, part]
        scores = (nt(q, k) * local[h]).astype(BF16)
        cum = cumb[h]
        end = cum[rows - 1 : rows, :]
        weighted = (k.astype(F32) * jnp.exp(end - cum)).astype(BF16)
        fresh[h] = dot(weighted.T, v)
        running[h] = dot(scores, v)
    for h in range(heads):
        local[h, :, pl.ds(0, HEAD_DIM)] = running[h]
    running[...] = jnp.zeros_like(running)
    trailing[...] = jnp.zeros_like(trailing)

    def stick(b, diagonal):
        def one(r, carry):
            at_r = pl.ds(pl.multiple_of(r * chunk, chunk), chunk)
            for h in range(heads):
                part = pl.ds(h * HEAD_DIM, HEAD_DIM)
                logits = nt(sq[at_r, part], kv[b, 0, :, part]) * scale + bias[h]
                soft = jnp.log(1.0 + jnp.exp(-jnp.abs(logits)))
                success = jnp.minimum(logits, 0.0) - soft
                failure = -jnp.maximum(logits, 0.0) - soft
                if diagonal:
                    seen = lax.broadcasted_iota(jnp.int32, (chunk, rows), 1) < (
                        lax.broadcasted_iota(jnp.int32, (chunk, rows), 0) + r * chunk
                    )
                    failure = jnp.where(seen, failure, 0.0)
                high = failure.astype(BF16)
                low = (failure - high.astype(F32)).astype(BF16)
                suffix = dot(high, tri[...]) + dot(low, tri[...])
                weights = jnp.exp(success + suffix)
                if diagonal:
                    weights = jnp.where(seen, weights, 0.0)
                partial = dot(weights.astype(BF16), kv[b, 1, :, part])
                behind = trailing[h, at_r, :]
                running[h, at_r, :] += jnp.exp(behind) * partial
                trailing[h, at_r, :] = behind + jnp.broadcast_to(
                    suffix[:, 0:1] + failure[:, 0:1], (chunk, HEAD_DIM)
                )
            return carry

        lax.fori_loop(0, chunks, one, 0)

    def chain():
        arriving = remote(st_out, st_in, st_s, st_r, me + 1, t)

        @pl.when(me > 0)
        def _():
            arriving.wait_recv()

        @pl.when(me == 0)
        def _():
            st_in[...] = jnp.zeros_like(st_in)

        @pl.when(me + 1 < shards)
        def _():
            for h in range(heads):
                end = cumb[h, pl.ds(rows - 1, 1), :]
                st_out[h] = (jnp.exp(end) * st_in[h].astype(F32) + fresh[h]).astype(BF16)
            arriving.start()

        for h in range(heads):
            carried = dot(qrot[h], st_in[h]) * jnp.exp(cumb[h])
            feats[:, pl.ds(h * HEAD_DIM, HEAD_DIM)] = head_norm(
                local[h, :, pl.ds(0, HEAD_DIM)] + carried
            ).astype(BF16)

    stick(me, True)
    moment = jnp.maximum(me - 1, 0)

    @pl.when(moment == 0)
    def _():
        chain()

    def visit(s, carry):
        b = me - s
        block_copy(b, 0, me).wait_recv()
        spread(b, lambda copy: copy.start())
        stick(b, False)

        @pl.when(s == moment)
        def _():
            chain()

        return carry

    lax.fori_loop(1, me + 1, visit, 0)

    for h in range(heads):
        feats[:, pl.ds(width + h * HEAD_DIM, HEAD_DIM)] = head_norm(running[h]).astype(BF16)

    for load in out_loads:
        load.wait()
    offs = tuple(range(1, chips)) + (0,)

    def project(r, target):
        columns = pl.ds(pl.multiple_of(target * depth, depth), depth)
        return dot(feats[pl.ds(r * chunk, chunk), :], wo[:, columns])

    def pair_copy(off, r):
        cut = pl.ds(r * chunk, chunk)
        return remote(
            d_send.at[off, cut, :], d_recv.at[off, cut, :], dd_s.at[off, r], dd_r.at[off, r], me, partner
        )

    def far_copy(off, r):
        cut = pl.ds(r * chunk, chunk)
        return remote(
            y_send.at[off, cut, :],
            y_recv.at[off, cut, :],
            yy_s.at[off, r],
            yy_r.at[off, r],
            me,
            tp_at(off),
        )

    for off in offs:
        for r in range(chunks):
            target = tp_at(off) // CORES * CORES + (1 - core)
            d_send[off, pl.ds(r * chunk, chunk), :] = project(r, target).astype(BF16)
            pair_copy(off, r).start()
    for off in offs:
        for r in range(chunks):
            cut = pl.ds(r * chunk, chunk)
            value = project(r, tp_at(off))
            pair_copy(off, r).wait_recv()
            value = value + d_recv[off, cut, :].astype(F32)
            if off:
                y_send[off, cut, :] = value.astype(BF16)
                far_copy(off, r).start()
            else:
                acc[cut, pl.ds(0, depth)] = value
    for r in range(chunks):
        cut = pl.ds(r * chunk, chunk)
        value = acc[cut, pl.ds(0, depth)]
        for off in range(1, chips):
            far_copy(off, r).wait_recv()
            value = value + y_recv[off, cut, :].astype(F32)
        out[cut, :] = value.astype(BF16)

    near.wait_send()
    for copy in sends + forwards:
        copy.wait_send()

    def drain(s, carry):
        spread(me - s, lambda copy: copy.wait_send())
        return carry

    lax.fori_loop(0, me + 1, drain, 0)

    @pl.when(me + 1 < shards)
    def _():
        remote(st_out, st_in, st_s, st_r, me + 1, t).wait_send()

    for off in offs:
        for r in range(chunks):
            pair_copy(off, r).wait_send()
            if off:
                far_copy(off, r).wait_send()


def body(
    tokens,
    ret_query,
    ret_key,
    ret_value,
    stick_query,
    stick_key,
    stick_value,
    log_decay,
    stick_bias,
    out_ret,
    out_stick,
):
    shards, parts = lax.axis_size("sp"), lax.axis_size("tp")
    rows, depth = tokens.shape
    width = ret_query.shape[1]
    heads = width // HEAD_DIM
    chips = parts // CORES
    across = row_width(shards)
    chunk = 128 if rows % 128 == 0 else rows
    chunks = rows // chunk
    half = HEAD_DIM // 2
    positions = (lax.axis_index("sp") * rows + jnp.arange(rows, dtype=jnp.int32)).astype(F32)
    inverse = ROPE_BASE ** (-jnp.arange(half, dtype=F32) / half)
    angles = positions[:, None] * inverse[None, :]
    cosine, sine = jnp.cos(angles), jnp.sin(angles)
    cos_t = jnp.concatenate([cosine, cosine], axis=1)
    sin_t = jnp.concatenate([-sine, sine], axis=1)
    any_spec = pl.BlockSpec(memory_space=pl.ANY)
    vmem = pl.BlockSpec(memory_space=pltpu.VMEM)
    dma = pltpu.SemaphoreType.DMA
    return pl.pallas_call(
        functools.partial(kernel, shards, parts),
        out_shape=jax.ShapeDtypeStruct((rows, depth), BF16),
        in_specs=[any_spec] * 9 + [vmem] * 3 + [pl.BlockSpec(memory_space=pltpu.SMEM)],
        out_specs=vmem,
        scratch_shapes=[
            pltpu.VMEM((parts, rows, depth), BF16),
            pltpu.VMEM((parts * depth, 6 * width), BF16),
            pltpu.VMEM((2 * width, parts * depth), BF16),
            pltpu.VMEM((rows, max(6 * width, heads * rows, depth)), F32),
            pltpu.VMEM((shards, 2, rows, width), BF16),
            pltpu.VMEM((rows, width), BF16),
            pltpu.VMEM((heads, rows, HEAD_DIM), BF16),
            pltpu.VMEM((rows, width), BF16),
            pltpu.VMEM((heads, rows, rows), F32),
            pltpu.VMEM((rows, rows), BF16),
            pltpu.VMEM((heads, rows, HEAD_DIM), F32),
            pltpu.VMEM((heads, HEAD_DIM, HEAD_DIM), F32),
            pltpu.VMEM((heads, HEAD_DIM, HEAD_DIM), BF16),
            pltpu.VMEM((heads, HEAD_DIM, HEAD_DIM), BF16),
            pltpu.VMEM((heads, rows, HEAD_DIM), F32),
            pltpu.VMEM((heads, rows, HEAD_DIM), F32),
            pltpu.VMEM((rows, 2 * width), BF16),
            pltpu.VMEM((chips, rows, depth), BF16),
            pltpu.VMEM((chips, rows, depth), BF16),
            pltpu.VMEM((chips, rows, depth), BF16),
            pltpu.VMEM((chips, rows, depth), BF16),
            dma((8,)),
            dma,
            dma((chips,)),
            dma((chips,)),
            dma((chips,)),
            dma((chips,)),
            dma((shards, across)),
            dma((shards,)),
            dma,
            dma,
            dma((chips, chunks)),
            dma((chips, chunks)),
            dma((chips, chunks)),
            dma((chips, chunks)),
        ],
        compiler_params=pltpu.CompilerParams(
            collective_id=0, has_side_effects=True, vmem_limit_bytes=60000 * 1024
        ),
    )(
        tokens,
        ret_query,
        ret_key,
        ret_value,
        stick_query,
        stick_key,
        stick_value,
        out_ret,
        out_stick,
        log_decay,
        cos_t,
        sin_t,
        stick_bias,
    )


def solution(mesh):
    in_specs = (
        P("sp", "tp"),
        P(None, "tp"),
        P(None, "tp"),
        P(None, "tp"),
        P(None, "tp"),
        P(None, "tp"),
        P(None, "tp"),
        P("sp", "tp"),
        P("tp"),
        P("tp", None),
        P("tp", None),
    )
    return jax.shard_map(
        body, mesh=mesh, in_specs=in_specs, out_specs=P("sp", "tp"), check_vma=False
    )
```

```python
import functools

import jax
import jax.numpy as jnp
from jax import lax
from jax.experimental import pallas as pl
from jax.experimental.pallas import tpu as pltpu
from jax.sharding import PartitionSpec as P

HEAD_DIM = 128
EPS = 1e-05
ROPE_BASE = 10000.0
CORES = 2
F32 = jnp.float32
BF16 = jnp.bfloat16


def row_width(shards):
    width = 1
    while (2 * width) ** 2 <= shards and shards % (2 * width) == 0:
        width *= 2
    return width


def head_norm(values):
    centred = values - jnp.mean(values, axis=-1, keepdims=True)
    spread = jnp.mean(centred * centred, axis=-1, keepdims=True)
    return centred * lax.rsqrt(spread + EPS)


def nt(a, b):
    return lax.dot_general(a, b, (((1,), (1,)), ((), ())), preferred_element_type=F32)


def dot(a, b):
    return jnp.dot(a, b, preferred_element_type=F32)


def kernel(
    shards,
    parts,
    tok,
    w_rq,
    w_rk,
    w_rv,
    w_sq,
    w_sk,
    w_sv,
    o_ret,
    o_stick,
    log_decay,
    cos_t,
    sin_t,
    bias,
    out,
    xs,
    wall,
    wo,
    acc,
    kv,
    sq,
    qrot,
    retv,
    local,
    tri,
    cumb,
    fresh,
    st_in,
    st_out,
    running,
    trailing,
    feats,
    d_send,
    d_recv,
    y_send,
    y_recv,
    w_sem,
    tok_sem,
    own_s,
    own_r,
    fwd_s,
    fwd_r,
    kv_s,
    kv_r,
    st_s,
    st_r,
    dd_s,
    dd_r,
    yy_s,
    yy_r,
):
    rows, depth = tok.shape
    width = w_rq.shape[1]
    heads = width // HEAD_DIM
    chips = parts // CORES
    across = row_width(shards)
    me = lax.axis_index("sp")
    t = lax.axis_index("tp")
    chip = t // CORES
    core = t % CORES
    partner = chip * CORES + (1 - core)
    column = me % across
    first = me - column
    chunk = 128 if rows % 128 == 0 else rows
    chunks = rows // chunk
    scale = HEAD_DIM ** (-0.5)

    def tp_at(off):
        return lax.rem(chip + off + chips, chips) * CORES + core

    def at(sp_index, tp_index):
        return {"sp": sp_index, "tp": tp_index}

    order = (w_sk, w_sv, w_sq, w_rk, w_rv, w_rq)
    own_load = pltpu.make_async_copy(tok, xs.at[t], tok_sem)
    own_load.start()
    loads = []
    for i, w in enumerate(order):
        load = pltpu.make_async_copy(w, wall.at[:, pl.ds(i * width, width)], w_sem.at[i])
        load.start()
        loads.append(load)
    out_loads = []
    for i, w in enumerate((o_ret, o_stick)):
        load = pltpu.make_async_copy(w, wo.at[pl.ds(i * width, width), :], w_sem.at[6 + i])
        load.start()
        out_loads.append(load)

    barrier = pltpu.get_barrier_semaphore()

    def greet(sp_index, tp_index):
        pl.semaphore_signal(
            barrier, inc=1, device_id=at(sp_index, tp_index), device_id_type=pl.DeviceIdType.MESH
        )

    greet(me, partner)
    for off in range(1, chips):
        greet(me, tp_at(off))
    for off in range(1, across):
        greet(first + lax.rem(column + off, across), t)
    count = 1 + (chips - 1) + (across - 1)
    for step in (across, 1):
        up = me + step < shards
        down = me - step >= 0

        @pl.when(up)
        def _():
            greet(me + step, t)

        @pl.when(down)
        def _():
            greet(me - step, t)

        count = count + up.astype(jnp.int32) + down.astype(jnp.int32)
    pl.semaphore_wait(barrier, count)

    def remote(src, dst, send, recv, sp_index, tp_index):
        return pltpu.make_async_remote_copy(
            src_ref=src,
            dst_ref=dst,
            send_sem=send,
            recv_sem=recv,
            device_id=at(sp_index, tp_index),
            device_id_type=pl.DeviceIdType.MESH,
        )

    sends = []
    for off in range(1, chips):
        copy = remote(tok, xs.at[t], own_s.at[off], own_r.at[off], me, tp_at(off))
        copy.start()
        sends.append(copy)
    near = remote(tok, xs.at[t], own_s.at[0], own_r.at[0], me, partner)
    near.start()

    lane = lax.broadcasted_iota(jnp.int32, (rows, rows), 1)
    sub = lax.broadcasted_iota(jnp.int32, (rows, rows), 0)
    tri[...] = (sub > lane).astype(BF16)
    for h in range(heads):
        column_ld = jnp.broadcast_to(log_decay[:, h : h + 1], (rows, rows))
        cum_row = jnp.sum(jnp.where(sub <= lane, column_ld, 0.0), axis=0, keepdims=True)
        ld_row = jnp.sum(jnp.where(sub == lane, column_ld, 0.0), axis=0, keepdims=True)
        cum_col = jnp.sum(
            jnp.where(lane <= sub, jnp.broadcast_to(ld_row, (rows, rows)), 0.0),
            axis=1,
            keepdims=True,
        )
        gaps = cum_col - cum_row
        acc[:, pl.ds(h * rows, rows)] = jnp.where(
            lane <= sub, jnp.exp(jnp.where(lane <= sub, gaps, 0.0)), 0.0
        )
        cumb[h] = jnp.broadcast_to(cum_col, (rows, HEAD_DIM))
    for h in range(heads):
        local[h] = acc[:, pl.ds(h * rows, rows)]

    own_load.wait()
    for load in loads:
        load.wait()

    def weight(j, lo, size):
        return wall[pl.ds(pl.multiple_of(j * depth, depth), depth), pl.ds(lo, size)]

    total = 6 * width
    for i in range(3):
        lo = i * 2 * width
        acc[:, pl.ds(lo, 2 * width)] = dot(xs[t], weight(t, lo, 2 * width))
    near.wait_recv()
    for i in range(3):
        lo = i * 2 * width
        acc[:, pl.ds(lo, 2 * width)] += dot(xs[partner], weight(partner, lo, 2 * width))
    forwards = []
    for off in range(1, chips):
        sends[off - 1].wait_recv()
        j = tp_at(-off)
        copy = remote(xs.at[j], xs.at[j], fwd_s.at[off], fwd_r.at[off], me, partner)
        copy.start()
        forwards.append(copy)
        for i in range(3):
            lo = i * 2 * width
            acc[:, pl.ds(lo, 2 * width)] += dot(xs[j], weight(j, lo, 2 * width))
    far = []
    for off in range(1, chips):
        forwards[off - 1].wait_recv()
        j = tp_at(-off) // CORES * CORES + (1 - core)
        far.append(j)

    def finish(lo, size):
        value = acc[:, pl.ds(lo, size)]
        for j in far:
            value = value + dot(xs[j], weight(j, lo, size))
        return value

    kv[me, 0] = finish(0, width).astype(BF16)
    kv[me, 1] = finish(width, width).astype(BF16)

    def block_copy(b, slot, target):
        return remote(kv.at[b], kv.at[b], kv_s.at[b, slot], kv_r.at[b], target, t)

    def spread(b, act):
        mine = lax.rem(b, across) == column

        @pl.when(jnp.logical_and(mine, me + across < shards))
        def _():
            act(block_copy(b, 0, me + across))

        for off in range(1, across):
            target = first + lax.rem(column + off, across)

            @pl.when(jnp.logical_and(mine, jnp.logical_or(b < me, target > me)))
            def _():
                act(block_copy(b, off, target))

    spread(me, lambda copy: copy.start())

    sq[...] = finish(2 * width, width).astype(BF16)
    rk = finish(3 * width, width).astype(BF16).astype(F32)
    retv[...] = finish(4 * width, width).astype(BF16)
    rq = finish(5 * width, width).astype(BF16).astype(F32)
    cos, sin = cos_t[...], sin_t[...]
    for h in range(heads):
        part = slice(h * HEAD_DIM, (h + 1) * HEAD_DIM)
        q, k = rq[:, part], rk[:, part]
        q = (q * cos + pltpu.roll(q, HEAD_DIM // 2, 1) * sin).astype(BF16)
        k = ((k * cos + pltpu.roll(k, HEAD_DIM // 2, 1) * sin) * scale).astype(BF16)
        qrot[h] = q
        v = retv[:, part]
        scores = (nt(q, k) * local[h]).astype(BF16)
        cum = cumb[h]
        end = cum[rows - 1 : rows, :]
        weighted = (k.astype(F32) * jnp.exp(end - cum)).astype(BF16)
        fresh[h] = dot(weighted.T, v)
        running[h] = dot(scores, v)
    for h in range(heads):
        local[h, :, pl.ds(0, HEAD_DIM)] = running[h]
    running[...] = jnp.zeros_like(running)
    trailing[...] = jnp.zeros_like(trailing)

    def stick(b, diagonal, chunk=rows, chunks=1):
        def one(r, carry):
            at_r = pl.ds(pl.multiple_of(r * chunk, chunk), chunk)
            for h in range(heads):
                part = pl.ds(h * HEAD_DIM, HEAD_DIM)
                logits = nt(sq[at_r, part], kv[b, 0, :, part]) * scale + bias[h]
                soft = jnp.log(1.0 + jnp.exp(-jnp.abs(logits)))
                success = jnp.minimum(logits, 0.0) - soft
                failure = -jnp.maximum(logits, 0.0) - soft
                if diagonal:
                    seen = lax.broadcasted_iota(jnp.int32, (chunk, rows), 1) < (
                        lax.broadcasted_iota(jnp.int32, (chunk, rows), 0) + r * chunk
                    )
                    failure = jnp.where(seen, failure, 0.0)
                high = failure.astype(BF16)
                low = (failure - high.astype(F32)).astype(BF16)
                suffix = dot(high, tri[...]) + dot(low, tri[...])
                weights = jnp.exp(success + suffix)
                if diagonal:
                    weights = jnp.where(seen, weights, 0.0)
                partial = dot(weights.astype(BF16), kv[b, 1, :, part])
                behind = trailing[h, at_r, :]
                running[h, at_r, :] += jnp.exp(behind) * partial
                trailing[h, at_r, :] = behind + jnp.broadcast_to(
                    suffix[:, 0:1] + failure[:, 0:1], (chunk, HEAD_DIM)
                )
            return carry

        lax.fori_loop(0, chunks, one, 0)

    def chain():
        arriving = remote(st_out, st_in, st_s, st_r, me + 1, t)

        @pl.when(me > 0)
        def _():
            arriving.wait_recv()

        @pl.when(me == 0)
        def _():
            st_in[...] = jnp.zeros_like(st_in)

        @pl.when(me + 1 < shards)
        def _():
            for h in range(heads):
                end = cumb[h, pl.ds(rows - 1, 1), :]
                st_out[h] = (jnp.exp(end) * st_in[h].astype(F32) + fresh[h]).astype(BF16)
            arriving.start()

        for h in range(heads):
            carried = dot(qrot[h], st_in[h]) * jnp.exp(cumb[h])
            feats[:, pl.ds(h * HEAD_DIM, HEAD_DIM)] = head_norm(
                local[h, :, pl.ds(0, HEAD_DIM)] + carried
            ).astype(BF16)

    stick(me, True)
    plane = me // across

    def visit(s, carry):
        k, i = s // across, lax.rem(s, across)
        b = (plane - k) * across + (across - 1 - i)

        @pl.when(jnp.logical_and(i == 0, k < plane))
        def _():
            nxt = me - (k + 1) * across
            block_copy(nxt, 0, me).wait_recv()
            spread(nxt, lambda copy: copy.start())

        @pl.when(jnp.logical_and(k == plane, i == column))
        def _():
            chain()

        @pl.when(jnp.logical_and(b < me, lax.rem(b, across) != column))
        def _():
            block_copy(b, 0, me).wait_recv()

        @pl.when(b < me)
        def _():
            stick(b, False)

        return carry

    lax.fori_loop(0, (plane + 1) * across, visit, 0)

    for h in range(heads):
        feats[:, pl.ds(width + h * HEAD_DIM, HEAD_DIM)] = head_norm(running[h]).astype(BF16)

    for load in out_loads:
        load.wait()
    offs = tuple(range(1, chips)) + (0,)

    def project(r, target):
        columns = pl.ds(pl.multiple_of(target * depth, depth), depth)
        return dot(feats[pl.ds(r * chunk, chunk), :], wo[:, columns])

    def pair_copy(off, r):
        cut = pl.ds(r * chunk, chunk)
        return remote(
            d_send.at[off, cut, :], d_recv.at[off, cut, :], dd_s.at[off, r], dd_r.at[off, r], me, partner
        )

    def far_copy(off, r):
        cut = pl.ds(r * chunk, chunk)
        return remote(
            y_send.at[off, cut, :],
            y_recv.at[off, cut, :],
            yy_s.at[off, r],
            yy_r.at[off, r],
            me,
            tp_at(off),
        )

    for off in offs:
        for r in range(chunks):
            target = tp_at(off) // CORES * CORES + (1 - core)
            d_send[off, pl.ds(r * chunk, chunk), :] = project(r, target).astype(BF16)
            pair_copy(off, r).start()
    for off in offs:
        for r in range(chunks):
            cut = pl.ds(r * chunk, chunk)
            value = project(r, tp_at(off))
            pair_copy(off, r).wait_recv()
            value = value + d_recv[off, cut, :].astype(F32)
            if off:
                y_send[off, cut, :] = value.astype(BF16)
                far_copy(off, r).start()
            else:
                acc[cut, pl.ds(0, depth)] = value
    for r in range(chunks):
        cut = pl.ds(r * chunk, chunk)
        value = acc[cut, pl.ds(0, depth)]
        for off in range(1, chips):
            far_copy(off, r).wait_recv()
            value = value + y_recv[off, cut, :].astype(F32)
        out[cut, :] = value.astype(BF16)

    near.wait_send()
    for copy in sends + forwards:
        copy.wait_send()

    def drain(s, carry):
        spread(me - s, lambda copy: copy.wait_send())
        return carry

    lax.fori_loop(0, me + 1, drain, 0)

    @pl.when(me + 1 < shards)
    def _():
        remote(st_out, st_in, st_s, st_r, me + 1, t).wait_send()

    for off in offs:
        for r in range(chunks):
            pair_copy(off, r).wait_send()
            if off:
                far_copy(off, r).wait_send()


def body(
    tokens,
    ret_query,
    ret_key,
    ret_value,
    stick_query,
    stick_key,
    stick_value,
    log_decay,
    stick_bias,
    out_ret,
    out_stick,
):
    shards, parts = lax.axis_size("sp"), lax.axis_size("tp")
    rows, depth = tokens.shape
    width = ret_query.shape[1]
    heads = width // HEAD_DIM
    chips = parts // CORES
    across = row_width(shards)
    chunk = 128 if rows % 128 == 0 else rows
    chunks = rows // chunk
    half = HEAD_DIM // 2
    positions = (lax.axis_index("sp") * rows + jnp.arange(rows, dtype=jnp.int32)).astype(F32)
    inverse = ROPE_BASE ** (-jnp.arange(half, dtype=F32) / half)
    angles = positions[:, None] * inverse[None, :]
    cosine, sine = jnp.cos(angles), jnp.sin(angles)
    cos_t = jnp.concatenate([cosine, cosine], axis=1)
    sin_t = jnp.concatenate([-sine, sine], axis=1)
    any_spec = pl.BlockSpec(memory_space=pl.ANY)
    vmem = pl.BlockSpec(memory_space=pltpu.VMEM)
    dma = pltpu.SemaphoreType.DMA
    return pl.pallas_call(
        functools.partial(kernel, shards, parts),
        out_shape=jax.ShapeDtypeStruct((rows, depth), BF16),
        in_specs=[any_spec] * 9 + [vmem] * 3 + [pl.BlockSpec(memory_space=pltpu.SMEM)],
        out_specs=vmem,
        scratch_shapes=[
            pltpu.VMEM((parts, rows, depth), BF16),
            pltpu.VMEM((parts * depth, 6 * width), BF16),
            pltpu.VMEM((2 * width, parts * depth), BF16),
            pltpu.VMEM((rows, max(6 * width, heads * rows, depth)), F32),
            pltpu.VMEM((shards, 2, rows, width), BF16),
            pltpu.VMEM((rows, width), BF16),
            pltpu.VMEM((heads, rows, HEAD_DIM), BF16),
            pltpu.VMEM((rows, width), BF16),
            pltpu.VMEM((heads, rows, rows), F32),
            pltpu.VMEM((rows, rows), BF16),
            pltpu.VMEM((heads, rows, HEAD_DIM), F32),
            pltpu.VMEM((heads, HEAD_DIM, HEAD_DIM), F32),
            pltpu.VMEM((heads, HEAD_DIM, HEAD_DIM), BF16),
            pltpu.VMEM((heads, HEAD_DIM, HEAD_DIM), BF16),
            pltpu.VMEM((heads, rows, HEAD_DIM), F32),
            pltpu.VMEM((heads, rows, HEAD_DIM), F32),
            pltpu.VMEM((rows, 2 * width), BF16),
            pltpu.VMEM((chips, rows, depth), BF16),
            pltpu.VMEM((chips, rows, depth), BF16),
            pltpu.VMEM((chips, rows, depth), BF16),
            pltpu.VMEM((chips, rows, depth), BF16),
            dma((8,)),
            dma,
            dma((chips,)),
            dma((chips,)),
            dma((chips,)),
            dma((chips,)),
            dma((shards, across)),
            dma((shards,)),
            dma,
            dma,
            dma((chips, chunks)),
            dma((chips, chunks)),
            dma((chips, chunks)),
            dma((chips, chunks)),
        ],
        compiler_params=pltpu.CompilerParams(
            collective_id=0, has_side_effects=True, vmem_limit_bytes=60000 * 1024
        ),
    )(
        tokens,
        ret_query,
        ret_key,
        ret_value,
        stick_query,
        stick_key,
        stick_value,
        out_ret,
        out_stick,
        log_decay,
        cos_t,
        sin_t,
        stick_bias,
    )


def solution(mesh):
    in_specs = (
        P("sp", "tp"),
        P(None, "tp"),
        P(None, "tp"),
        P(None, "tp"),
        P(None, "tp"),
        P(None, "tp"),
        P(None, "tp"),
        P("sp", "tp"),
        P("tp"),
        P("tp", None),
        P("tp", None),
    )
    return jax.shard_map(
        body, mesh=mesh, in_specs=in_specs, out_specs=P("sp", "tp"), check_vma=False
    )
```

```python
import functools

import jax
import jax.numpy as jnp
import numpy as np
from jax import lax
from jax.experimental import pallas as pl
from jax.experimental.pallas import tpu as pltpu
from jax.sharding import PartitionSpec as P

HEAD_DIM = 128
EPS = 1e-05
ROPE_BASE = 10000.0
CORES = 2
F32 = jnp.float32
BF16 = jnp.bfloat16


def row_width(shards):
    width = 1
    while (2 * width) ** 2 <= shards and shards % (2 * width) == 0:
        width *= 2
    return width


def head_norm(values):
    centred = values - jnp.mean(values, axis=-1, keepdims=True)
    spread = jnp.mean(centred * centred, axis=-1, keepdims=True)
    return centred * lax.rsqrt(spread + EPS)


def nt(a, b):
    return lax.dot_general(a, b, (((1,), (1,)), ((), ())), preferred_element_type=F32)


def dot(a, b):
    return jnp.dot(a, b, preferred_element_type=F32)


def kernel(
    shards,
    parts,
    tok,
    w_rq,
    w_rk,
    w_rv,
    w_sq,
    w_sk,
    w_sv,
    o_ret,
    o_stick,
    log_decay,
    inverse,
    bias,
    out,
    xs,
    wall,
    wo,
    acc,
    kv,
    sq,
    qrot,
    retv,
    local,
    tri,
    cumb,
    fresh,
    st_in,
    st_out,
    running,
    trailing,
    feats,
    turn,
    d_send,
    d_recv,
    y_send,
    y_recv,
    w_sem,
    tok_sem,
    own_s,
    own_r,
    fwd_s,
    fwd_r,
    kv_s,
    kv_r,
    st_s,
    st_r,
    dd_s,
    dd_r,
    yy_s,
    yy_r,
):
    rows, depth = tok.shape
    width = w_rq.shape[1]
    heads = width // HEAD_DIM
    chips = parts // CORES
    across = row_width(shards)
    me = lax.axis_index("sp")
    t = lax.axis_index("tp")
    chip = t // CORES
    core = t % CORES
    partner = chip * CORES + (1 - core)
    column = me % across
    first = me - column
    chunk = 128 if rows % 128 == 0 else rows
    chunks = rows // chunk
    scale = HEAD_DIM ** (-0.5)

    def tp_at(off):
        return lax.rem(chip + off + chips, chips) * CORES + core

    def at(sp_index, tp_index):
        return {"sp": sp_index, "tp": tp_index}

    order = (w_sk, w_sv, w_sq, w_rk, w_rv, w_rq)
    own_load = pltpu.make_async_copy(tok, xs.at[t], tok_sem)
    own_load.start()
    loads = []
    for i, w in enumerate(order):
        load = pltpu.make_async_copy(w, wall.at[:, pl.ds(i * width, width)], w_sem.at[i])
        load.start()
        loads.append(load)
    out_loads = []
    for i, w in enumerate((o_ret, o_stick)):
        load = pltpu.make_async_copy(w, wo.at[pl.ds(i * width, width), :], w_sem.at[6 + i])
        load.start()
        out_loads.append(load)

    barrier = pltpu.get_barrier_semaphore()

    def greet(sp_index, tp_index):
        pl.semaphore_signal(
            barrier, inc=1, device_id=at(sp_index, tp_index), device_id_type=pl.DeviceIdType.MESH
        )

    greet(me, partner)
    for off in range(1, chips):
        greet(me, tp_at(off))
    for off in range(1, across):
        greet(first + lax.rem(column + off, across), t)
    count = 1 + (chips - 1) + (across - 1)
    for step in (across, 1):
        up = me + step < shards
        down = me - step >= 0

        @pl.when(up)
        def _():
            greet(me + step, t)

        @pl.when(down)
        def _():
            greet(me - step, t)

        count = count + up.astype(jnp.int32) + down.astype(jnp.int32)
    pl.semaphore_wait(barrier, count)

    def remote(src, dst, send, recv, sp_index, tp_index):
        return pltpu.make_async_remote_copy(
            src_ref=src,
            dst_ref=dst,
            send_sem=send,
            recv_sem=recv,
            device_id=at(sp_index, tp_index),
            device_id_type=pl.DeviceIdType.MESH,
        )

    sends = []
    for off in range(1, chips):
        copy = remote(tok, xs.at[t], own_s.at[off], own_r.at[off], me, tp_at(off))
        copy.start()
        sends.append(copy)
    near = remote(tok, xs.at[t], own_s.at[0], own_r.at[0], me, partner)
    near.start()

    lane = lax.broadcasted_iota(jnp.int32, (rows, rows), 1)
    sub = lax.broadcasted_iota(jnp.int32, (rows, rows), 0)
    tri[...] = (sub > lane).astype(BF16)
    for h in range(heads):
        column_ld = jnp.broadcast_to(log_decay[:, h : h + 1], (rows, rows))
        cum_row = jnp.sum(jnp.where(sub <= lane, column_ld, 0.0), axis=0, keepdims=True)
        ld_row = jnp.sum(jnp.where(sub == lane, column_ld, 0.0), axis=0, keepdims=True)
        cum_col = jnp.sum(
            jnp.where(lane <= sub, jnp.broadcast_to(ld_row, (rows, rows)), 0.0),
            axis=1,
            keepdims=True,
        )
        gaps = cum_col - cum_row
        acc[:, pl.ds(h * rows, rows)] = jnp.where(
            lane <= sub, jnp.exp(jnp.where(lane <= sub, gaps, 0.0)), 0.0
        )
        cumb[h] = jnp.broadcast_to(cum_col, (rows, HEAD_DIM))
    for h in range(heads):
        local[h] = acc[:, pl.ds(h * rows, rows)]

    angles = (
        me * rows + lax.broadcasted_iota(jnp.int32, (rows, HEAD_DIM), 0)
    ).astype(F32) * inverse[...]
    left = lax.broadcasted_iota(jnp.int32, (rows, HEAD_DIM), 1) < HEAD_DIM // 2
    sine = jnp.sin(angles)
    turn[0] = jnp.cos(angles)
    turn[1] = jnp.where(left, -sine, sine)

    own_load.wait()
    for load in loads:
        load.wait()

    def weight(j, lo, size):
        return wall[pl.ds(pl.multiple_of(j * depth, depth), depth), pl.ds(lo, size)]

    total = 6 * width
    for i in range(3):
        lo = i * 2 * width
        acc[:, pl.ds(lo, 2 * width)] = dot(xs[t], weight(t, lo, 2 * width))
    near.wait_recv()
    for i in range(3):
        lo = i * 2 * width
        acc[:, pl.ds(lo, 2 * width)] += dot(xs[partner], weight(partner, lo, 2 * width))
    forwards = []
    for off in range(1, chips):
        sends[off - 1].wait_recv()
        j = tp_at(-off)
        copy = remote(xs.at[j], xs.at[j], fwd_s.at[off], fwd_r.at[off], me, partner)
        copy.start()
        forwards.append(copy)
        for i in range(3):
            lo = i * 2 * width
            acc[:, pl.ds(lo, 2 * width)] += dot(xs[j], weight(j, lo, 2 * width))
    far = []
    for off in range(1, chips):
        forwards[off - 1].wait_recv()
        j = tp_at(-off) // CORES * CORES + (1 - core)
        far.append(j)

    def finish(lo, size):
        value = acc[:, pl.ds(lo, size)]
        for j in far:
            value = value + dot(xs[j], weight(j, lo, size))
        return value

    for i in range(2):
        value = finish(i * width, width).astype(BF16)
        for h in range(heads):
            kv[me, h, i] = value[:, h * HEAD_DIM : (h + 1) * HEAD_DIM]

    def block_copy(b, h, slot, target):
        return remote(
            kv.at[b, h], kv.at[b, h], kv_s.at[b, slot, h], kv_r.at[b, h], target, t
        )

    def spread(b, h, act):
        mine = lax.rem(b, across) == column

        @pl.when(jnp.logical_and(mine, me + across < shards))
        def _():
            act(block_copy(b, h, 0, me + across))

        for off in range(1, across):
            target = first + lax.rem(column + off, across)

            @pl.when(jnp.logical_and(mine, jnp.logical_or(b < me, target > me)))
            def _():
                act(block_copy(b, h, off, target))

    for h in range(heads):
        spread(me, h, lambda copy: copy.start())

    sq[...] = finish(2 * width, width).astype(BF16)
    rk = finish(3 * width, width).astype(BF16).astype(F32)
    retv[...] = finish(4 * width, width).astype(BF16)
    rq = finish(5 * width, width).astype(BF16).astype(F32)
    cos, sin = turn[0], turn[1]
    for h in range(heads):
        part = slice(h * HEAD_DIM, (h + 1) * HEAD_DIM)
        q, k = rq[:, part], rk[:, part]
        q = (q * cos + pltpu.roll(q, HEAD_DIM // 2, 1) * sin).astype(BF16)
        k = ((k * cos + pltpu.roll(k, HEAD_DIM // 2, 1) * sin) * scale).astype(BF16)
        qrot[h] = q
        v = retv[:, part]
        scores = (nt(q, k) * local[h]).astype(BF16)
        cum = cumb[h]
        end = cum[rows - 1 : rows, :]
        weighted = (k.astype(F32) * jnp.exp(end - cum)).astype(BF16)
        fresh[h] = dot(weighted.T, v)
        running[h] = dot(scores, v)
    for h in range(heads):
        local[h, :, pl.ds(0, HEAD_DIM)] = running[h]
    running[...] = jnp.zeros_like(running)
    trailing[...] = jnp.zeros_like(trailing)

    def stick(b, diagonal, chunk=rows, chunks=1):
        def one(r, carry):
            at_r = pl.ds(r * chunk, chunk)
            for h in range(heads):
                if not diagonal:

                    @pl.when(lax.rem(b, across) != column)
                    def _():
                        block_copy(b, h, 0, me).wait_recv()

                part = pl.ds(h * HEAD_DIM, HEAD_DIM)
                logits = nt(sq[at_r, part], kv[b, h, 0]) * scale + bias[h]
                soft = jnp.log(1.0 + jnp.exp(-jnp.abs(logits)))
                success = jnp.minimum(logits, 0.0) - soft
                failure = -jnp.maximum(logits, 0.0) - soft
                if diagonal:
                    seen = lax.broadcasted_iota(jnp.int32, (chunk, rows), 1) < (
                        lax.broadcasted_iota(jnp.int32, (chunk, rows), 0) + r * chunk
                    )
                    failure = jnp.where(seen, failure, 0.0)
                high = failure.astype(BF16)
                low = (failure - high.astype(F32)).astype(BF16)
                suffix = dot(high, tri[...]) + dot(low, tri[...])
                weights = jnp.exp(success + suffix)
                if diagonal:
                    weights = jnp.where(seen, weights, 0.0)
                partial = dot(weights.astype(BF16), kv[b, h, 1])
                behind = trailing[h, at_r, :]
                running[h, at_r, :] += jnp.exp(behind) * partial
                trailing[h, at_r, :] = behind + jnp.broadcast_to(
                    suffix[:, 0:1] + failure[:, 0:1], (chunk, HEAD_DIM)
                )
            return carry

        one(0, 0)

    def chain():
        arriving = remote(st_out, st_in, st_s, st_r, me + 1, t)

        @pl.when(me > 0)
        def _():
            arriving.wait_recv()

        @pl.when(me == 0)
        def _():
            st_in[...] = jnp.zeros_like(st_in)

        @pl.when(me + 1 < shards)
        def _():
            for h in range(heads):
                end = cumb[h, pl.ds(rows - 1, 1), :]
                st_out[h] = (jnp.exp(end) * st_in[h].astype(F32) + fresh[h]).astype(BF16)
            arriving.start()

        for h in range(heads):
            carried = dot(qrot[h], st_in[h]) * jnp.exp(cumb[h])
            feats[:, pl.ds(h * HEAD_DIM, HEAD_DIM)] = head_norm(
                local[h, :, pl.ds(0, HEAD_DIM)] + carried
            ).astype(BF16)

    stick(me, True)
    plane = me // across

    def visit(s, carry):
        k, i = s // across, lax.rem(s, across)
        b = (plane - k) * across + (across - 1 - i)

        @pl.when(jnp.logical_and(i == 0, k < plane))
        def _():
            nxt = me - (k + 1) * across
            for h in range(heads):
                block_copy(nxt, h, 0, me).wait_recv()
                spread(nxt, h, lambda copy: copy.start())

        @pl.when(jnp.logical_and(k == plane, i == column))
        def _():
            chain()

        @pl.when(b < me)
        def _():
            stick(b, False)

        return carry

    lax.fori_loop(0, (plane + 1) * across, visit, 0)

    for h in range(heads):
        feats[:, pl.ds(width + h * HEAD_DIM, HEAD_DIM)] = head_norm(running[h]).astype(BF16)

    for load in out_loads:
        load.wait()
    offs = tuple(range(1, chips)) + (0,)

    def project(r, target):
        columns = pl.ds(pl.multiple_of(target * depth, depth), depth)
        return dot(feats[pl.ds(r * chunk, chunk), :], wo[:, columns])

    def pair_copy(off, r):
        cut = pl.ds(r * chunk, chunk)
        return remote(
            d_send.at[off, cut, :], d_recv.at[off, cut, :], dd_s.at[off, r], dd_r.at[off, r], me, partner
        )

    def far_copy(off, r):
        cut = pl.ds(r * chunk, chunk)
        return remote(
            y_send.at[off, cut, :],
            y_recv.at[off, cut, :],
            yy_s.at[off, r],
            yy_r.at[off, r],
            me,
            tp_at(off),
        )

    def send_half(off):
        target = tp_at(off) // CORES * CORES + (1 - core)
        for r in range(chunks):
            d_send[off, pl.ds(r * chunk, chunk), :] = project(r, target).astype(BF16)
            pair_copy(off, r).start()

    send_half(offs[0])
    for n, off in enumerate(offs):
        for r in range(chunks):
            cut = pl.ds(r * chunk, chunk)
            value = project(r, tp_at(off))
            pair_copy(off, r).wait_recv()
            value = value + d_recv[off, cut, :].astype(F32)
            if off:
                y_send[off, cut, :] = value.astype(BF16)
                far_copy(off, r).start()
            else:
                acc[cut, pl.ds(0, depth)] = value
        if n + 1 < len(offs):
            send_half(offs[n + 1])
    for r in range(chunks):
        cut = pl.ds(r * chunk, chunk)
        value = acc[cut, pl.ds(0, depth)]
        for off in range(1, chips):
            far_copy(off, r).wait_recv()
            value = value + y_recv[off, cut, :].astype(F32)
        out[cut, :] = value.astype(BF16)

    near.wait_send()
    for copy in sends + forwards:
        copy.wait_send()

    def drain(s, carry):
        for h in range(heads):
            spread(me - s, h, lambda copy: copy.wait_send())
        return carry

    lax.fori_loop(0, me + 1, drain, 0)

    @pl.when(me + 1 < shards)
    def _():
        remote(st_out, st_in, st_s, st_r, me + 1, t).wait_send()

    for off in offs:
        for r in range(chunks):
            pair_copy(off, r).wait_send()
            if off:
                far_copy(off, r).wait_send()


def body(
    tokens,
    ret_query,
    ret_key,
    ret_value,
    stick_query,
    stick_key,
    stick_value,
    log_decay,
    stick_bias,
    out_ret,
    out_stick,
):
    shards, parts = lax.axis_size("sp"), lax.axis_size("tp")
    rows, depth = tokens.shape
    width = ret_query.shape[1]
    heads = width // HEAD_DIM
    chips = parts // CORES
    across = row_width(shards)
    chunk = 128 if rows % 128 == 0 else rows
    chunks = rows // chunk
    half = HEAD_DIM // 2
    inverse = np.float32(ROPE_BASE) ** (-np.arange(half, dtype=np.float32) / np.float32(half))
    inverse = jnp.asarray(np.tile(inverse, 2)[None, :], F32)
    any_spec = pl.BlockSpec(memory_space=pl.ANY)
    vmem = pl.BlockSpec(memory_space=pltpu.VMEM)
    dma = pltpu.SemaphoreType.DMA
    return pl.pallas_call(
        functools.partial(kernel, shards, parts),
        out_shape=jax.ShapeDtypeStruct((rows, depth), BF16),
        in_specs=[any_spec] * 9 + [vmem] * 2 + [pl.BlockSpec(memory_space=pltpu.SMEM)],
        out_specs=vmem,
        scratch_shapes=[
            pltpu.VMEM((parts, rows, depth), BF16),
            pltpu.VMEM((parts * depth, 6 * width), BF16),
            pltpu.VMEM((2 * width, parts * depth), BF16),
            pltpu.VMEM((rows, max(6 * width, heads * rows, depth)), F32),
            pltpu.VMEM((shards, heads, 2, rows, HEAD_DIM), BF16),
            pltpu.VMEM((rows, width), BF16),
            pltpu.VMEM((heads, rows, HEAD_DIM), BF16),
            pltpu.VMEM((rows, width), BF16),
            pltpu.VMEM((heads, rows, rows), F32),
            pltpu.VMEM((rows, rows), BF16),
            pltpu.VMEM((heads, rows, HEAD_DIM), F32),
            pltpu.VMEM((heads, HEAD_DIM, HEAD_DIM), F32),
            pltpu.VMEM((heads, HEAD_DIM, HEAD_DIM), BF16),
            pltpu.VMEM((heads, HEAD_DIM, HEAD_DIM), BF16),
            pltpu.VMEM((heads, rows, HEAD_DIM), F32),
            pltpu.VMEM((heads, rows, HEAD_DIM), F32),
            pltpu.VMEM((rows, 2 * width), BF16),
            pltpu.VMEM((2, rows, HEAD_DIM), F32),
            pltpu.VMEM((chips, rows, depth), BF16),
            pltpu.VMEM((chips, rows, depth), BF16),
            pltpu.VMEM((chips, rows, depth), BF16),
            pltpu.VMEM((chips, rows, depth), BF16),
            dma((8,)),
            dma,
            dma((chips,)),
            dma((chips,)),
            dma((chips,)),
            dma((chips,)),
            dma((shards, across, heads)),
            dma((shards, heads)),
            dma,
            dma,
            dma((chips, chunks)),
            dma((chips, chunks)),
            dma((chips, chunks)),
            dma((chips, chunks)),
        ],
        compiler_params=pltpu.CompilerParams(
            collective_id=0, has_side_effects=True, vmem_limit_bytes=60000 * 1024
        ),
    )(
        tokens,
        ret_query,
        ret_key,
        ret_value,
        stick_query,
        stick_key,
        stick_value,
        out_ret,
        out_stick,
        log_decay,
        inverse,
        stick_bias,
    )


def solution(mesh):
    in_specs = (
        P("sp", "tp"),
        P(None, "tp"),
        P(None, "tp"),
        P(None, "tp"),
        P(None, "tp"),
        P(None, "tp"),
        P(None, "tp"),
        P("sp", "tp"),
        P("tp"),
        P("tp", None),
        P("tp", None),
    )
    return jax.shard_map(
        body, mesh=mesh, in_specs=in_specs, out_specs=P("sp", "tp"), check_vma=False
    )
```
